512 devices in a mesh: sp: 64 (over z, y), dp: 8 (over x, core).
Axes of the slice: x: 4, y: 4, z: 16, core: 2. Of those that a mesh axis runs over, the one named last changes fastest.
Arguments:
- signal: bfloat16 [8, 8192, 1024], P('dp', 'sp'), may hold values from -6 to 6
- pace: float32 [8, 64], P('dp'), may hold values from 0.5 to 2
- log_step: float32 [64], P('sp'), may hold values from -5.52 to -4.42
- a_real: float32 [64, 64], P('sp'), may hold values from -4 to -0.002, as said below
- a_imag: float32 [64, 64], P('sp'), may hold values from 0.5 to 201.06177
- in_map: float32 [64, 2, 64, 16], P('sp'), may hold values from -3 to 3
- out_map: float32 [64, 2, 16, 64], P('sp'), may hold values from -0.5 to 0.5
- skip: float32 [1024], P('sp'), may hold values from -1 to 1
- init_state: float32 [8, 2, 64, 64], P('dp', None, 'sp'), may hold values from -5 to 5
- w_glu: bfloat16 [1024, 1024], P('sp', 'dp'), may hold values from -0.1875 to 0.1875
- b_glu: float32 [1024], replicated, may hold values from -4 to 4
- g_mix: float32 [1024], replicated, may hold values from 0.1 to 1.9
- w_out: bfloat16 [1024, 4096], P('sp', 'dp'), may hold values from -0.1875 to 0.1875
Outputs:
- result: bfloat16 [8, 8192, 4096], P('dp', 'sp')
The draws below stay inside these ranges and needn't reach their ends.
Inputs may be any that keep to these rules, and one draw needn't show every extreme that they name: `a_real`: negative entries; within a group all entries are of one order.
All inputs are finite; a program needn't handle non-finite values.
Results may differ from the reference program's by a relative error of at most 0.0075.
Values may be sent and summed in bfloat16 or wider, within the bound.
A program may use at most 64 MiB of HBM per device.

```python
import math
import jax
import jax.numpy as jnp
from jax import lax

D = 4096
GROUPS = 64
C = 16
P_SIZE = 64
WIDTH = 1024
LENGTH = 8192
BATCH = 8
SPANS = 64


def draw_a_real(key, part):
    first, second, third = jax.random.split(key, 3)
    share = 0.5
    slow = jax.random.uniform(first, (GROUPS, 1), jnp.float32) < share
    slow_rate = jax.random.uniform(second, (GROUPS, P_SIZE), jnp.float32, 0.002, 0.006)
    fast_rate = jax.random.uniform(third, (GROUPS, P_SIZE), jnp.float32, 1.5, 4.0)
    return -jnp.where(slow, slow_rate, fast_rate)


def block_scale(own_key, extent, pieces, low, high):
    def one(axis_at, shards_of):
        steps = jax.random.uniform(jax.random.fold_in(jax.random.fold_in(own_key, 6), axis_at), (shards_of,), jnp.float32, low / len(pieces), high / len(pieces))
        return jnp.repeat(jnp.exp(steps), extent[axis_at] // shards_of).reshape((-1,) + (1,) * (len(extent) - axis_at - 1))

    level = one(*pieces[0])
    for cut in pieces[1:]:
        level = level * one(*cut)
    return level


def scatter_about(own_key, extent, width, reach, pieces=(), kind=jnp.bfloat16):
    factor_of = block_scale(own_key, extent, pieces, -0.22, 0.18) if pieces else 1.0
    result = jax.random.normal(own_key, extent, jnp.float32) * width * factor_of
    return jnp.minimum(jnp.maximum(result, -reach), reach).astype(kind)


def setup_inputs(seed: int = 0) -> dict:
    seeds = jax.random.split(jax.random.key(seed), 14)
    return {
        "signal": scatter_about(seeds[0], (BATCH, LENGTH, WIDTH), 1.0, 6.0, ((0, 8), (1, 64))),
        "pace": jnp.clip(jnp.exp(math.log(2.0) - 1.3862944 * jax.random.uniform(seeds[1], (BATCH, SPANS), jnp.float32) ** block_scale(seeds[1], (BATCH, SPANS), ((0, 8),), -0.2, 0.2)), 0.5, 2.0),
        "log_step": jnp.clip(-5.52 + 1.0999999 * jax.random.uniform(seeds[2], (GROUPS,), jnp.float32) ** block_scale(seeds[2], (GROUPS,), ((0, 64),), -0.2, 0.2), -5.52, -4.42),
        "a_real": draw_a_real(jax.random.fold_in(seeds[13], 71), 0),
        "a_imag": jnp.clip(0.5 + 200.56177 * jax.random.uniform(seeds[4], (GROUPS, P_SIZE), jnp.float32) ** block_scale(seeds[4], (GROUPS, P_SIZE), ((0, 64),), -0.2, 0.2), 0.5, 201.06177),
        "in_map": scatter_about(seeds[5], (GROUPS, 2, P_SIZE, C), 0.5, 3.0, ((0, 64),), jnp.float32),
        "out_map": scatter_about(seeds[6], (GROUPS, 2, C, P_SIZE), (2 * P_SIZE) ** -0.5, 0.5, ((0, 64),), jnp.float32),
        "skip": jnp.clip(jax.random.uniform(seeds[7], (WIDTH,), jnp.float32, -1.0, 1.0) * block_scale(seeds[7], (WIDTH,), ((0, 64),), -0.4, 0.0), -1.0, 1.0),
        "init_state": scatter_about(seeds[8], (BATCH, 2, GROUPS, P_SIZE), 1.0, 5.0, ((0, 8), (2, 64)), jnp.float32),
        "w_glu": scatter_about(seeds[9], (WIDTH, WIDTH), WIDTH ** -0.5, 0.1875, ((0, 64), (1, 8))),
        "b_glu": scatter_about(seeds[10], (WIDTH,), 1.0, 4.0, (), jnp.float32),
        "g_mix": jnp.clip(1.0 + 0.18 * jax.random.normal(seeds[11], (WIDTH,), jnp.float32), 0.1, 1.9),
        "w_out": scatter_about(seeds[12], (WIDTH, D), WIDTH ** -0.5, 0.1875, ((0, 64), (1, 8))),
    }


def combine(first, second):
    a1r, a1i, b1r, b1i = first
    a2r, a2i, b2r, b2i = second
    return (a2r * a1r - a2i * a1i, a2r * a1i + a2i * a1r, a2r * b1r - a2i * b1i + b2r, a2r * b1i + a2i * b1r + b2i)

def mix_group(series, pace_row, log_rate, a_re, a_im, in_map, out_map, skip_row, init):
    blocks_count = pace_row.shape[0]
    length = series.shape[0]
    span = length // blocks_count
    states = a_re.shape[0]
    steps = (jnp.exp(log_rate) * pace_row)[:, None]
    decay = jnp.exp(a_re * steps)
    bar_re = decay * jnp.cos(a_im * steps)
    bar_im = decay * jnp.sin(a_im * steps)
    modulus = a_re * a_re + a_im * a_im
    coef_re = ((bar_re - 1.0) * a_re + bar_im * a_im) / modulus
    coef_im = (bar_im * a_re - (bar_re - 1.0) * a_im) / modulus
    drive_re = coef_re[..., None] * in_map[0] - coef_im[..., None] * in_map[1]
    drive_im = coef_re[..., None] * in_map[1] + coef_im[..., None] * in_map[0]
    drive = jnp.concatenate([drive_re, drive_im], axis=1).astype(jnp.bfloat16)
    blocks = series.reshape(blocks_count, span, series.shape[1])
    inject = jnp.einsum('ksc,kpc->ksp', blocks.astype(jnp.float32), drive.astype(jnp.float32))
    inject = inject.reshape(length, 2 * states)
    in_re = inject[:, :states]
    in_im = inject[:, states:]
    in_re = in_re.at[0].add(bar_re[0] * init[0] - bar_im[0] * init[1])
    in_im = in_im.at[0].add(bar_re[0] * init[1] + bar_im[0] * init[0])
    step_re = jnp.broadcast_to(bar_re[:, None, :], (blocks_count, span, states)).reshape(length, states)
    step_im = jnp.broadcast_to(bar_im[:, None, :], (blocks_count, span, states)).reshape(length, states)
    scanned = lax.associative_scan(combine, (step_re, step_im, in_re, in_im), axis=0)
    highest = lax.Precision.HIGHEST
    response = jnp.dot(scanned[2], out_map[0].T, precision=highest) - jnp.dot(scanned[3], out_map[1].T, precision=highest)
    response = response + skip_row * series.astype(jnp.float32)
    return jax.nn.gelu(response).astype(jnp.bfloat16)

def reference(signal, pace, log_step, a_real, a_imag, in_map, out_map, skip, init_state, w_glu, b_glu, g_mix, w_out):
    grouped = signal.reshape(BATCH, LENGTH, GROUPS, C)
    skips = skip.reshape(GROUPS, C)

    def per_sequence(index):
        sample = lax.dynamic_index_in_dim(grouped, index, 0, keepdims=False)
        pace_row = lax.dynamic_index_in_dim(pace, index, 0, keepdims=False)
        init_row = lax.dynamic_index_in_dim(init_state, index, 0, keepdims=False)

        def per_group(group):
            series = lax.dynamic_index_in_dim(sample, group, 1, keepdims=False)
            start = lax.dynamic_index_in_dim(init_row, group, 1, keepdims=False)
            return mix_group(series, pace_row, log_step[group], a_real[group], a_imag[group], in_map[group], out_map[group], skips[group], start)
        outputs = lax.map(per_group, jnp.arange(GROUPS, dtype=jnp.int32))
        activated = outputs.transpose(1, 0, 2).reshape(LENGTH, WIDTH)
        gate_pre = jnp.dot(activated, w_glu, preferred_element_type=jnp.float32) + b_glu
        gated = activated.astype(jnp.float32) * jax.nn.sigmoid(gate_pre)
        scale = lax.rsqrt(lax.optimization_barrier(jnp.mean(gated * gated, axis=-1, keepdims=True)) + 1e-06)
        mixed = (gated * scale * g_mix).astype(jnp.bfloat16)
        return jnp.dot(mixed, w_out, preferred_element_type=jnp.float32).astype(jnp.bfloat16)
    return lax.map(per_sequence, jnp.arange(BATCH, dtype=jnp.int32))
```

```python
import jax
import jax.numpy as jnp
from jax import lax
from jax.experimental import pallas as pl
from jax.experimental.pallas import tpu as pltpu
from jax.sharding import Mesh
from jax.sharding import PartitionSpec as P

NZ, NY, NX, NC = 16, 4, 4, 2
SPN = NZ * NY
SP = ("z", "y")
DP = ("x", "c")
HALF = NZ // 2
F32 = jnp.float32
BF16 = jnp.bfloat16
MESH = pl.DeviceIdType.MESH


def cmul(ar, ai, br, bi):
    return ar * br - ai * bi, ar * bi + ai * br


def body(
    sig, wg, wo, rhs_in, lhs_out, skip, step, are, aim, init, bglu, gmix,
    out,
    W, UT, U, Vr, Vi, ASend, ARecv, Br, Bi, mixed, gpre, obuf,
    loc, rps, rpr, rms, rmr, ays, ayr, axs, axr, ads, adr,
    bxs, bxr, bys, byr, bds, bdr, us, ur, vs, vr, osem,
):
    z = lax.axis_index("z")
    y = lax.axis_index("y")
    x = lax.axis_index("x")
    c = lax.axis_index("c")
    me = z * NY + y
    zp, zm = lax.rem(z + 1, NZ), lax.rem(z + NZ - 1, NZ)
    yp, ym, y2 = lax.rem(y + 1, NY), lax.rem(y + NY - 1, NY), lax.rem(y + 2, NY)
    xp, xm, x2 = lax.rem(x + 1, NX), lax.rem(x + NX - 1, NX), lax.rem(x + 2, NX)
    other = 1 - c

    def dev(zz=None, yy=None, xx=None, cc=None):
        return (
            z if zz is None else zz,
            y if yy is None else yy,
            x if xx is None else xx,
            c if cc is None else cc,
        )

    def rcopy(ref, ss, rs, to):
        return pltpu.make_async_remote_copy(
            src_ref=ref, dst_ref=ref, send_sem=ss, recv_sem=rs, device_id=to, device_id_type=MESH
        )

    barrier = pltpu.get_barrier_semaphore()

    def greet(d, carry):
        peer = lax.rem(me + d, SPN)
        pl.semaphore_signal(
            barrier, inc=1, device_id=dev(peer // NY, lax.rem(peer, NY)), device_id_type=MESH
        )
        return carry

    lax.fori_loop(1, SPN, greet, 0)
    for to in (dev(xx=xp), dev(xx=xm), dev(cc=other)):
        pl.semaphore_signal(barrier, inc=1, device_id=to, device_id_type=MESH)

    own = W.at[c, x, z, y]
    load_o = pltpu.make_async_copy(wo, own.at[:, pl.ds(0, 512)], loc.at[0])
    load_g = pltpu.make_async_copy(wg, own.at[:, pl.ds(512, 128)], loc.at[1])
    load_o.start()
    load_g.start()
    for b in range(8):
        piece = sig[0, :, b * 128 : (b + 1) * 128]
        UT[b * 8 : (b + 1) * 8] = piece.T.reshape(8, 16, 128)
    U[me] = UT[me]
    load_o.wait()
    load_g.wait()
    pl.semaphore_wait(barrier, SPN - 1 + 3)

    sent = []

    def push(copy):
        copy.start()
        sent.append(copy)

    def arrive(ref, rs):
        rcopy(ref, rs, rs, dev(cc=other)).wait_recv()

    def ring(t):
        za, zb = lax.rem(z + NZ - t, NZ), lax.rem(z + t, NZ)
        if 0 < t < HALF:
            arrive(W.at[c, x, za, y], rpr.at[t])
        if t < HALF - 1:
            push(rcopy(W.at[c, x, za, y], rps.at[t + 1], rpr.at[t + 1], dev(zz=zp)))
        if 0 < t <= HALF:
            arrive(W.at[c, x, zb, y], rmr.at[t])
        if t < HALF:
            push(rcopy(W.at[c, x, zb, y], rms.at[t + 1], rmr.at[t + 1], dev(zz=zm)))

    def around(i, view, plus, minus, at, ss, rs, stage):
        p_at, m_at, o_at = at
        if stage == 0:
            push(rcopy(view(None), ss.at[i, 0], rs.at[i, 0], plus))
            push(rcopy(view(None), ss.at[i, 1], rs.at[i, 1], minus))
        elif stage == 1:
            arrive(view(m_at), rs.at[i, 0])
            arrive(view(p_at), rs.at[i, 1])
            if i % 2 == 0:
                push(rcopy(view(m_at), ss.at[i, 2], rs.at[i, 2], plus))
            else:
                push(rcopy(view(p_at), ss.at[i, 2], rs.at[i, 2], minus))
        else:
            arrive(view(o_at), rs.at[i, 2])

    ysides = (dev(yy=yp), dev(yy=ym), (yp, ym, y2))
    xsides = (dev(xx=xp), dev(xx=xm), (xp, xm, x2))

    def chain_a(i, s):
        za = lax.rem(z + NZ - i, NZ)
        one = lambda at: W.at[c, x, za, y if at is None else at]
        row = lambda at: W.at[c, x if at is None else at, za]
        if s <= 1:
            around(i, one, *ysides, ays, ayr, s)
        elif s == 2:
            around(i, one, *ysides, ays, ayr, 2)
            around(i, row, *xsides, axs, axr, 0)
        elif s == 3:
            around(i, row, *xsides, axs, axr, 1)
        elif s == 4:
            around(i, row, *xsides, axs, axr, 2)
            push(rcopy(W.at[c, pl.ds(0, NX), za], ads.at[i], adr.at[i], dev(cc=other)))

    def chain_b(i, s):
        zb = lax.rem(z + 1 + i, NZ)
        one = lambda at: W.at[c, x if at is None else at, zb, y]
        col = lambda at: W.at[c, pl.ds(0, NX), zb, y if at is None else at]
        if s <= 1:
            around(i, one, *xsides, bxs, bxr, s)
        elif s == 2:
            around(i, one, *xsides, bxs, bxr, 2)
            around(i, col, *ysides, bys, byr, 0)
        elif s == 3:
            around(i, col, *ysides, bys, byr, 1)
        elif s == 4:
            around(i, col, *ysides, bys, byr, 2)
            push(rcopy(W.at[c, pl.ds(0, NX), zb], bds.at[i], bdr.at[i], dev(cc=other)))

    def advance(t):
        if t <= HALF:
            ring(t)
        for s in range(5):
            if 0 <= t - s < HALF:
                chain_a(t - s, s)
            if 0 <= t - 1 - s < HALF:
                chain_b(t - 1 - s, s)

    def to_peer(src, dst, ss, rs, peer):
        return pltpu.make_async_remote_copy(
            src_ref=src.at[peer],
            dst_ref=dst.at[me],
            send_sem=ss.at[peer],
            recv_sem=rs.at[me],
            device_id=dev(peer // NY, lax.rem(peer, NY)),
            device_id_type=MESH,
        )

    def from_peer(src, dst, ss, rs, peer):
        return pltpu.make_async_remote_copy(
            src_ref=src.at[peer],
            dst_ref=dst.at[peer],
            send_sem=ss.at[peer],
            recv_sem=rs.at[peer],
            device_id=dev(peer // NY, lax.rem(peer, NY)),
            device_id_type=MESH,
        )

    def every_peer(act):
        def one(d, carry):
            act(lax.rem(me + d, SPN))
            return carry

        lax.fori_loop(1, SPN, one, 0)

    advance(0)
    every_peer(lambda p: to_peer(UT, U, us, ur, p).start())
    for t in range(1, HALF + 1):
        advance(t)
    every_peer(lambda p: from_peer(UT, U, us, ur, p).wait_recv())

    st = step[...]
    decay = jnp.exp(are[...] * st)
    angle = aim[...] * st
    bar_r = decay * jnp.cos(angle)
    bar_i = decay * jnp.sin(angle)
    modulus = are[...] * are[...] + aim[...] * aim[...]
    co_r = ((bar_r - 1.0) * are[...] + bar_i * aim[...]) / modulus
    co_i = (bar_i * are[...] - (bar_r - 1.0) * aim[...]) / modulus

    def inject(a, carry):
        for j in range(8):
            r = a * 8 + j
            pair = jnp.concatenate([U[r], U[r + 32]], axis=0)
            v = lax.dot_general(
                pair, rhs_in[...], (((0,), (0,)), ((), ())), preferred_element_type=F32
            )
            Vr[a, :, j, :] = v[:, :128]
            Vi[a, :, j, :] = v[:, 128:]
        return carry

    lax.fori_loop(0, 4, inject, 0)

    def parts(m):
        return [m[a * 8 : (a + 1) * 8] for a in range(4)]

    bars = list(zip(parts(bar_r), parts(bar_i)))
    coefs = list(zip(parts(co_r), parts(co_i)))

    def first_pass(s8, carry):
        carry = list(carry)
        for q in range(8):
            s = s8 * 8 + q
            for a in range(4):
                zr, zi = cmul(*bars[a], *carry[a])
                carry[a] = (zr + Vr[a, s], zi + Vi[a, s])
        return tuple(carry)

    zero = jnp.zeros((8, 128), F32)
    ends = lax.fori_loop(0, 16, first_pass, ((zero, zero),) * 4)
    er = jnp.concatenate([e[0] for e in ends], axis=0)
    ei = jnp.concatenate([e[1] for e in ends], axis=0)
    er, ei = cmul(co_r, co_i, er, ei)
    pr, pi = bar_r, bar_i
    for _ in range(7):
        pr, pi = cmul(pr, pi, pr, pi)
    row = lax.broadcasted_iota(jnp.int32, (32, 128), 0)
    for d in (1, 2, 4, 8, 16):
        keep = row >= d
        qr, qi = pltpu.roll(pr, d, 0), pltpu.roll(pi, d, 0)
        fr, fi = pltpu.roll(er, d, 0), pltpu.roll(ei, d, 0)
        gr, gi = cmul(pr, pi, fr, fi)
        hr, hi = cmul(pr, pi, qr, qi)
        er, ei = jnp.where(keep, er + gr, er), jnp.where(keep, ei + gi, ei)
        pr, pi = jnp.where(keep, hr, pr), jnp.where(keep, hi, pi)
    ir = jnp.broadcast_to(init[0:1], (8, 128))
    ii = jnp.broadcast_to(init[1:2], (8, 128))
    lr, li = cmul(pr[31:32], pi[31:32], ir, ii)
    lr, li = pltpu.roll(lr + er[31:32], 64, 1), pltpu.roll(li + ei[31:32], 64, 1)
    low = lax.broadcasted_iota(jnp.int32, (8, 128), 1) < 64
    sr, si = jnp.where(low, ir, lr)[0:1], jnp.where(low, ii, li)[0:1]
    br, bi = cmul(pr, pi, sr, si)
    br, bi = pltpu.roll(br + er, 1, 0), pltpu.roll(bi + ei, 1, 0)
    first = row == 0
    Br[...] = jnp.where(first, sr, br)
    Bi[...] = jnp.where(first, si, bi)

    def second_pass(s8, carry):
        carry = list(carry)
        for q in range(8):
            s = s8 * 8 + q
            for a in range(4):
                vr_, vi_ = cmul(*coefs[a], Vr[a, s], Vi[a, s])
                zr, zi = cmul(*bars[a], *carry[a])
                zr, zi = zr + vr_, zi + vi_
                Vr[a, s] = zr
                Vi[a, s] = zi
                carry[a] = (zr, zi)
        return tuple(carry)

    start = tuple((Br[a * 8 : (a + 1) * 8], Bi[a * 8 : (a + 1) * 8]) for a in range(4))
    lax.fori_loop(0, 16, second_pass, start)

    def respond(a, carry):
        for j in range(8):
            r = a * 8 + j
            state = jnp.concatenate(
                [Vr[a, :, j, :].astype(BF16), Vi[a, :, j, :].astype(BF16)], axis=1
            )
            pair = jnp.concatenate([U[r], U[r + 32]], axis=0)
            v = lax.dot_general(
                lhs_out[...], state, (((1,), (1,)), ((), ())), preferred_element_type=F32
            )
            v = v + skip[...] * pair.astype(F32)
            v = jax.nn.gelu(v).astype(BF16)
            ASend[r] = v[:16]
            ASend[r + 32] = v[16:]
        return carry

    lax.fori_loop(0, 4, respond, 0)
    ARecv[me] = ASend[me]
    every_peer(lambda p: to_peer(ASend, ARecv, vs, vr, p).start())
    for t in range(HALF + 1, HALF + 6):
        advance(t)
    every_peer(lambda p: from_peer(ASend, ARecv, vs, vr, p).wait_recv())
    for i in range(HALF):
        za, zb = lax.rem(z + NZ - i, NZ), lax.rem(z + 1 + i, NZ)
        arrive(W.at[other, pl.ds(0, NX), za], adr.at[i])
        arrive(W.at[other, pl.ds(0, NX), zb], bdr.at[i])

    for b in range(8):
        piece = ARecv[b * 8 : (b + 1) * 8].reshape(128, 128)
        mixed[:, b * 128 : (b + 1) * 128] = piece.T
    for d in range(8):
        gpre[:, d * 128 : (d + 1) * 128] = jnp.dot(
            mixed[...],
            W[d % 2, d // 2, :, :, :, 512:640].reshape(1024, 128),
            preferred_element_type=F32,
        )
    gated = mixed[...].astype(F32) * jax.nn.sigmoid(gpre[...] + bglu[...])
    scale = lax.rsqrt(jnp.mean(gated * gated, axis=-1, keepdims=True) + 1e-06)
    mixed[...] = (gated * scale * gmix[...]).astype(BF16)
    stores = []
    for d in range(8):
        obuf[d] = jnp.dot(
            mixed[...],
            W[d % 2, d // 2, :, :, :, 0:512].reshape(1024, 512),
            preferred_element_type=F32,
        ).astype(BF16)
        copy = pltpu.make_async_copy(obuf.at[d], out.at[0, :, pl.ds(d * 512, 512)], osem.at[d])
        copy.start()
        stores.append(copy)
    every_peer(lambda p: to_peer(UT, U, us, ur, p).wait_send())
    every_peer(lambda p: to_peer(ASend, ARecv, vs, vr, p).wait_send())
    for copy in sent:
        copy.wait_send()
    for copy in stores:
        copy.wait()


def per_device(
    signal, pace, log_step, a_real, a_imag, in_map, out_map, skip, init_state, w_glu, b_glu, g_mix, w_out
):
    step = jnp.exp(log_step[0]) * pace[0]
    step = jnp.repeat(step.reshape(2, 32).T, 64, axis=1)
    are = jnp.tile(a_real, (1, 2))
    aim = jnp.tile(a_imag, (1, 2))
    eye = jnp.eye(2, dtype=F32)
    inside = in_map[0].astype(BF16).astype(F32)
    rhs_in = jnp.einsum("rpc,gh->gcrhp", inside, eye).reshape(32, 256).astype(BF16)
    signs = jnp.array([1.0, -1.0], F32)[:, None, None]
    lhs_out = jnp.einsum("rcp,gh->gcrhp", out_map[0] * signs, eye).reshape(32, 256).astype(BF16)
    skips = jnp.broadcast_to(jnp.tile(skip, 2)[:, None], (32, 128))
    init = jnp.pad(init_state[0, :, 0, :], ((0, 0), (0, 64)))
    dma = pltpu.SemaphoreType.DMA
    vmem = pl.BlockSpec(memory_space=pltpu.VMEM)
    anywhere = pl.BlockSpec(memory_space=pl.ANY)
    return pl.pallas_call(
        body,
        out_shape=jax.ShapeDtypeStruct((1, 128, 4096), BF16),
        in_specs=[vmem, anywhere, anywhere] + [vmem] * 9,
        out_specs=anywhere,
        scratch_shapes=[
            pltpu.VMEM((NC, NX, NZ, NY, 16, 640), BF16),
            pltpu.VMEM((SPN, 16, 128), BF16),
            pltpu.VMEM((SPN, 16, 128), BF16),
            pltpu.VMEM((4, 128, 8, 128), F32),
            pltpu.VMEM((4, 128, 8, 128), F32),
            pltpu.VMEM((SPN, 16, 128), BF16),
            pltpu.VMEM((SPN, 16, 128), BF16),
            pltpu.VMEM((32, 128), F32),
            pltpu.VMEM((32, 128), F32),
            pltpu.VMEM((128, 1024), BF16),
            pltpu.VMEM((128, 1024), F32),
            pltpu.VMEM((8, 128, 512), BF16),
            dma((2,)),
            dma((9,)), dma((9,)), dma((9,)), dma((9,)),
            dma((8, 3)), dma((8, 3)), dma((8, 3)), dma((8, 3)), dma((8,)), dma((8,)),
            dma((8, 3)), dma((8, 3)), dma((8, 3)), dma((8, 3)), dma((8,)), dma((8,)),
            dma((SPN,)), dma((SPN,)), dma((SPN,)), dma((SPN,)),
            dma((8,)),
        ],
        compiler_params=pltpu.CompilerParams(
            collective_id=0, has_side_effects=True, vmem_limit_bytes=48 * 1024 * 1024
        ),
    )(signal, w_glu, w_out, rhs_in, lhs_out, skips, step, are, aim, init, b_glu[None], g_mix[None])


def solution(mesh):
    split = Mesh(mesh.devices.reshape(NZ, NY, NX, NC), ("z", "y", "x", "c"))
    placed = (
        P(DP, SP, None),
        P(DP, None),
        P(SP),
        P(SP, None),
        P(SP, None),
        P(SP, None, None, None),
        P(SP, None, None, None),
        P(SP),
        P(DP, None, SP, None),
        P(SP, DP),
        P(),
        P(),
        P(SP, DP),
    )
    return jax.shard_map(
        per_device, mesh=split, in_specs=placed, out_specs=P(DP, SP, None), check_vma=False
    )
```

```python
import jax
import jax.numpy as jnp
from jax import lax
from jax.experimental import pallas as pl
from jax.experimental.pallas import tpu as pltpu
from jax.sharding import Mesh
from jax.sharding import PartitionSpec as P

NZ, NY, NX, NC = 16, 4, 4, 2
SPN = NZ * NY
SP = ("z", "y")
DP = ("x", "c")
HALF = NZ // 2
F32 = jnp.float32
BF16 = jnp.bfloat16
MESH = pl.DeviceIdType.MESH


def cmul(ar, ai, br, bi):
    return ar * br - ai * bi, ar * bi + ai * br


def body(
    *args,
):
    inputs, out, copies, rest = args[:13], args[13], args[14:25], args[25:]
    body_of(*inputs[:3], *copies, inputs[3:], out, *rest)


def body_of(
    sig_hbm, wg, wo,
    sig, in_map, out_map, skip, pace, log_step, a_real, a_imag, init, bglu, gmix,
    small_hbm, out,
    W, UT, U, Vr, Vi, ASend, ARecv, Br, Bi, mixed, gpre, rows_in, rows_out, RJ, WJ, lanes,
    loc, sends, rpr, rmr, ayr, axr, bxr, byr, core, us, ur, vs, vr,
):
    z = lax.axis_index("z")
    y = lax.axis_index("y")
    x = lax.axis_index("x")
    c = lax.axis_index("c")
    me = z * NY + y
    zp, zm = lax.rem(z + 1, NZ), lax.rem(z + NZ - 1, NZ)
    yp, ym, y2 = lax.rem(y + 1, NY), lax.rem(y + NY - 1, NY), lax.rem(y + 2, NY)
    xp, xm, x2 = lax.rem(x + 1, NX), lax.rem(x + NX - 1, NX), lax.rem(x + 2, NX)
    other = 1 - c

    def dev(zz=None, yy=None, xx=None, cc=None):
        return (
            z if zz is None else zz,
            y if yy is None else yy,
            x if xx is None else xx,
            c if cc is None else cc,
        )

    def slot(zz, yy):
        return lax.rem(zz, HALF) * (2 * NY) + yy * 2 + zz // HALF

    def rcopy(ref, ss, rs, to):
        return pltpu.make_async_remote_copy(
            src_ref=ref, dst_ref=ref, send_sem=ss, recv_sem=rs, device_id=to, device_id_type=MESH
        )

    def every_peer(act):
        for dy in range(1, NY):
            act(z, lax.rem(y + dy, NY))

        def one(d, carry):
            zz = lax.rem(z + d, NZ)
            for dy in range(NY):
                act(zz, lax.rem(y + dy, NY))
            return carry

        lax.fori_loop(1, NZ, one, 0)

    load_sig = pltpu.make_async_copy(sig_hbm, sig, loc.at[2])
    load_sig.start()
    small = (in_map, out_map, skip, pace, log_step, a_real, a_imag, init, bglu, gmix)
    loads = []
    for n, (src, dst) in enumerate(zip(small_hbm, small, strict=True)):
        loads.append(pltpu.make_async_copy(src, dst, loc.at[3 + n]))
        loads[-1].start()
    barrier = pltpu.get_barrier_semaphore()

    def greet(to):
        pl.semaphore_signal(barrier, inc=1, device_id=to, device_id_type=MESH)

    with jax.named_scope("greet"):
        for to in (dev(xx=xp), dev(xx=xm), dev(cc=other)):
            greet(to)
        every_peer(lambda zz, yy: greet(dev(zz, yy)))

    with jax.named_scope("prepare"):
        own = W.at[c, x, z, y]
        load_o = pltpu.make_async_copy(wo, own.at[:, pl.ds(0, 512)], loc.at[0])
        load_g = pltpu.make_async_copy(wg, own.at[:, pl.ds(512, 128)], loc.at[1])
        load_o.start()
        load_g.start()
        load_sig.wait()
        for b in range(8):
            piece = sig[0, :, b * 128 : (b + 1) * 128]
            UT[b * 8 : (b + 1) * 8] = piece.T.reshape(8, 16, 128)
        U[slot(z, y)] = UT[me]
        for copy in loads:
            copy.wait()
        rows_in[...] = jnp.zeros((32, 256), F32)
        rows_out[...] = jnp.zeros((32, 256), F32)
        for g in range(2):
            for r in range(2):
                rs, cs = slice(g * 16, g * 16 + 16), slice(r * 128 + g * 64, r * 128 + g * 64 + 64)
                rows_in[rs, cs] = in_map[0, r]
                rows_out[rs, cs] = out_map[0, r] if r == 0 else -out_map[0, r]
            for n, ref in enumerate((a_real[0:1], a_imag[0:1], init[0, 0], init[0, 1])):
                lanes[n : n + 1, g * 64 : g * 64 + 64] = ref
        full_in = jnp.concatenate([rows_in[...]] * 8, axis=0)
        full_out = jnp.concatenate([rows_out[...]] * 8, axis=0).T
        row_of = lax.broadcasted_iota(jnp.int32, (256, 256), 0) // 32
        col_of = lax.broadcasted_iota(jnp.int32, (256, 256), 1) // 32
        for j in range(8):
            RJ[j] = jnp.where(row_of == j, full_in, 0.0).astype(BF16)
            WJ[j] = jnp.where(col_of == j, full_out, 0.0).astype(BF16)

        def column(line, count, offset):
            lane = lax.broadcasted_iota(jnp.int32, (count, line.shape[1]), 1)
            at = lax.broadcasted_iota(jnp.int32, (count, line.shape[1]), 0) + offset
            return jnp.sum(jnp.where(lane == at, line, 0.0), axis=1, keepdims=True)

        skips = jnp.broadcast_to(column(skip[...], 16, 0), (16, 128))[None]
        low32 = lax.broadcasted_iota(jnp.int32, (32, 128), 1) < 64
        line = pace[0:1]
        st = jnp.where(low32, column(line, 32, 0), column(line, 32, 32)) * jnp.exp(log_step[...])
        are, aim = lanes[0:1], lanes[1:2]
        decay = jnp.exp(are * st)
        angle = aim * st
        bar_r = decay * jnp.cos(angle)
        bar_i = decay * jnp.sin(angle)
        modulus = are * are + aim * aim
        co_r = ((bar_r - 1.0) * are + bar_i * aim) / modulus
        co_i = (bar_i * are - (bar_r - 1.0) * aim) / modulus
        pr, pi = bar_r, bar_i
        for _ in range(7):
            pr, pi = cmul(pr, pi, pr, pi)
    with jax.named_scope("barrier"):
        load_o.wait()
        load_g.wait()
        pl.semaphore_wait(barrier, SPN - 1 + 3)

    RING, NEAR, BULK, CORE = range(4)

    def push(ref, kind, rs, to):
        rcopy(ref, sends.at[kind], rs, to).start()

    def arrive(ref, rs):
        rcopy(ref, rs, rs, dev(cc=other)).wait_recv()

    def ring(t):
        za, zb = lax.rem(z + NZ - t, NZ), lax.rem(z + t, NZ)
        if 0 < t < HALF:
            arrive(W.at[c, x, za, y], rpr.at[t])
        if t < HALF - 1:
            push(W.at[c, x, za, y], RING, rpr.at[t + 1], dev(zz=zp))
        if 0 < t <= HALF:
            arrive(W.at[c, x, zb, y], rmr.at[t])
        if t < HALF:
            push(W.at[c, x, zb, y], RING, rmr.at[t + 1], dev(zz=zm))

    def around(i, view, pair, halves, kind, plus, minus, at, rs, stage):
        p_at, m_at, o_at = at
        if stage == 0:
            push(view(None), kind, rs.at[i, 0], plus)
            push(view(None), kind, rs.at[i, 0], minus)
        elif stage == 1:
            arrive(pair, rs.at[i, 0])
            push(halves[0](m_at), kind, rs.at[i, 1], plus)
            push(halves[1](p_at), kind, rs.at[i, 1], minus)
        else:
            arrive(view(o_at), rs.at[i, 1])

    ysides = (dev(yy=yp), dev(yy=ym), (yp, ym, y2))
    xsides = (dev(xx=xp), dev(xx=xm), (xp, xm, x2))

    def cut(view):
        return (
            lambda at: view(at).at[:, pl.ds(0, 384)],
            lambda at: view(at).at[:, pl.ds(384, 256)],
        )

    def chain_a(i, s):
        za = lax.rem(z + NZ - i, NZ)
        one = lambda at: W.at[c, x, za, y if at is None else at]
        row = lambda at: W.at[c, x if at is None else at, za]
        rows = (
            lambda at: W.at[c, at, za, pl.ds(0, 2)],
            lambda at: W.at[c, at, za, pl.ds(2, 2)],
        )
        if s <= 1:
            around(i, one, W.at[c, x, za, pl.ds(0, 2)], cut(one), NEAR, *ysides, ayr, s)
        elif s == 2:
            around(i, one, None, cut(one), NEAR, *ysides, ayr, 2)
            around(i, row, W.at[c, pl.ds(0, 2), za], rows, BULK, *xsides, axr, 0)
        elif s == 3:
            around(i, row, W.at[c, pl.ds(0, 2), za], rows, BULK, *xsides, axr, 1)
        elif s == 4:
            around(i, row, W.at[c, pl.ds(0, 2), za], rows, BULK, *xsides, axr, 2)
            push(W.at[c, pl.ds(0, NX), za], CORE, core.at[0], dev(cc=other))

    def chain_b(i, s):
        zb = lax.rem(z + 1 + i, NZ)
        one = lambda at: W.at[c, x if at is None else at, zb, y]
        col = lambda at: W.at[c, pl.ds(0, NX), zb, y if at is None else at]
        cols = (
            lambda at: W.at[c, pl.ds(0, 2), zb, at],
            lambda at: W.at[c, pl.ds(2, 2), zb, at],
        )
        if s <= 1:
            around(i, one, W.at[c, pl.ds(0, 2), zb, y], cut(one), NEAR, *xsides, bxr, s)
        elif s == 2:
            around(i, one, None, cut(one), NEAR, *xsides, bxr, 2)
            around(i, col, W.at[c, pl.ds(0, NX), zb, pl.ds(0, 2)], cols, BULK, *ysides, byr, 0)
        elif s == 3:
            around(i, col, W.at[c, pl.ds(0, NX), zb, pl.ds(0, 2)], cols, BULK, *ysides, byr, 1)
        elif s == 4:
            around(i, col, W.at[c, pl.ds(0, NX), zb, pl.ds(0, 2)], cols, BULK, *ysides, byr, 2)
            push(W.at[c, pl.ds(0, NX), zb], CORE, core.at[0], dev(cc=other))

    def advance(t):
        with jax.named_scope(f"t{t}"):
            if t <= HALF:
                ring(t)
            for s in range(5):
                if 0 <= t - s < HALF:
                    chain_a(t - s, s)
                if 0 <= t - 1 - s < HALF:
                    chain_b(t - 1 - s, s)

    def send_tile(src, dst, ss, rs, zz, yy):
        pltpu.make_async_remote_copy(
            src_ref=src,
            dst_ref=dst,
            send_sem=ss,
            recv_sem=rs,
            device_id=dev(zz, yy),
            device_id_type=MESH,
        ).start()

    def send_signal(dz):
        zz = lax.rem(z + dz + NZ, NZ)
        for dy in range(NY):
            if dz or dy:
                yy = lax.rem(y + dy, NY)
                send_tile(UT.at[zz * NY + yy], U.at[slot(z, y)], us.at[0], ur.at[0], zz, yy)

    def send_back(zz, yy):
        send_tile(ASend.at[slot(zz, yy)], ARecv.at[me], vs.at[0], vr.at[0], zz, yy)

    def all_tiles(ref, ss, rs):
        return rcopy(ref.at[pl.ds(0, SPN - 1)], ss, rs, dev(cc=other))

    for t, far in enumerate(((8,), (-7, 7), (-6, 6), (-5, 5), (-4, 4, -1, 1), (-3, 3, -2, 2, 0))):
        advance(t)
        with jax.named_scope("scatter"):
            for dz in far:
                send_signal(dz)
    advance(6)
    with jax.named_scope("await_signal"):
        all_tiles(U, us.at[0], ur.at[0]).wait_recv()

    with jax.named_scope("inject"):
        for a in range(4):
            for h in range(2):
                piece = U[a * 16 + h * 8 : a * 16 + h * 8 + 8].reshape(128, 128)
                mixed[:, a * 256 + h * 128 : a * 256 + h * 128 + 128] = piece.T

        def inject(a, carry):
            rows = mixed[:, pl.ds(pl.multiple_of(a * 256, 256), 256)]
            for j in range(8):
                v = jnp.dot(rows, RJ[j], preferred_element_type=F32)
                Vr[pl.ds(a * 1024 + j, 128, stride=8), :] = v[:, :128]
                Vi[pl.ds(a * 1024 + j, 128, stride=8), :] = v[:, 128:]
            return carry

        lax.fori_loop(0, 4, inject, 0)
    advance(7)

    def parts(m):
        return [m[a * 8 : (a + 1) * 8] for a in range(4)]

    bars = list(zip(parts(bar_r), parts(bar_i)))
    coefs = list(zip(parts(co_r), parts(co_i)))

    def first_pass(s8, carry):
        carry = list(carry)
        for q in range(8):
            s = s8 * 8 + q
            for a in range(4):
                at = pl.ds(pl.multiple_of(a * 1024 + s * 8, 8), 8)
                zr, zi = cmul(*bars[a], *carry[a])
                carry[a] = (zr + Vr[at], zi + Vi[at])
        return tuple(carry)

    zero = jnp.zeros((8, 128), F32)
    with jax.named_scope("first"):
        ends = lax.fori_loop(0, 16, first_pass, ((zero, zero),) * 4)
    er = jnp.concatenate([e[0] for e in ends], axis=0)
    ei = jnp.concatenate([e[1] for e in ends], axis=0)
    er, ei = cmul(co_r, co_i, er, ei)
    row = lax.broadcasted_iota(jnp.int32, (32, 128), 0)
    for d in (1, 2, 4, 8, 16):
        keep = row >= d
        qr, qi = pltpu.roll(pr, d, 0), pltpu.roll(pi, d, 0)
        fr, fi = pltpu.roll(er, d, 0), pltpu.roll(ei, d, 0)
        gr, gi = cmul(pr, pi, fr, fi)
        hr, hi = cmul(pr, pi, qr, qi)
        er, ei = jnp.where(keep, er + gr, er), jnp.where(keep, ei + gi, ei)
        pr, pi = jnp.where(keep, hr, pr), jnp.where(keep, hi, pi)
    ir = jnp.broadcast_to(lanes[2:3], (8, 128))
    ii = jnp.broadcast_to(lanes[3:4], (8, 128))
    lr, li = cmul(pr[31:32], pi[31:32], ir, ii)
    lr, li = pltpu.roll(lr + er[31:32], 64, 1), pltpu.roll(li + ei[31:32], 64, 1)
    low = lax.broadcasted_iota(jnp.int32, (8, 128), 1) < 64
    sr, si = jnp.where(low, ir, lr)[0:1], jnp.where(low, ii, li)[0:1]
    br, bi = cmul(pr, pi, sr, si)
    br, bi = pltpu.roll(br + er, 1, 0), pltpu.roll(bi + ei, 1, 0)
    Br[...] = jnp.where(row == 0, sr, br)
    Bi[...] = jnp.where(row == 0, si, bi)

    def second_pass(s8, carry):
        carry = list(carry)
        for q in range(8):
            s = s8 * 8 + q
            for a in range(4):
                at = pl.ds(pl.multiple_of(a * 1024 + s * 8, 8), 8)
                vr_, vi_ = cmul(*coefs[a], Vr[at], Vi[at])
                zr, zi = cmul(*bars[a], *carry[a])
                zr, zi = zr + vr_, zi + vi_
                Vr[at] = zr
                Vi[at] = zi
                carry[a] = (zr, zi)
        return tuple(carry)

    with jax.named_scope("second"):
        first = tuple((Br[a * 8 : (a + 1) * 8], Bi[a * 8 : (a + 1) * 8]) for a in range(4))
        lax.fori_loop(0, 16, second_pass, first)
    advance(8)

    with jax.named_scope("respond"):

        def respond(a, carry):
            total = jnp.zeros((128, 256), F32)
            for j in range(8):
                state = jnp.concatenate(
                    [ref[pl.ds(a * 1024 + j, 128, stride=8), :].astype(BF16) for ref in (Vr, Vi)], axis=1
                )
                total = total + jnp.dot(state, WJ[j], preferred_element_type=F32)
            for h in range(2):
                at = pl.ds(a * 16 + h * 8, 8)
                v = total[:, h * 128 : (h + 1) * 128].T.reshape(8, 16, 128)
                v = v + skips * U[at].astype(F32)
                ASend[at] = jax.nn.gelu(v).astype(BF16)
            return carry

        lax.fori_loop(0, 4, respond, 0)
    with jax.named_scope("scatter_back"):
        ARecv[me] = ASend[slot(z, y)]
        every_peer(send_back)
    for t in range(9, HALF + 6):
        advance(t)
    with jax.named_scope("await_activated"):
        all_tiles(ARecv, vs.at[0], vr.at[0]).wait_recv()
    with jax.named_scope("await_core"):
        arrive(W.at[other], core.at[0])

    with jax.named_scope("gate"):
        for b in range(8):
            piece = ARecv[b * 8 : (b + 1) * 8].reshape(128, 128)
            mixed[:, b * 128 : (b + 1) * 128] = piece.T
        for d in range(8):
            gpre[:, d * 128 : (d + 1) * 128] = jnp.dot(
                mixed[...],
                W[d % 2, d // 2, :, :, :, 512:640].reshape(1024, 128),
                preferred_element_type=F32,
            )
        gated = mixed[...].astype(F32) * jax.nn.sigmoid(gpre[...] + bglu[...])
        scale = lax.rsqrt(jnp.mean(gated * gated, axis=-1, keepdims=True) + 1e-06)
        mixed[...] = (gated * scale * gmix[...]).astype(BF16)
    with jax.named_scope("project"):
        for d in range(8):
            out[0, :, d * 512 : (d + 1) * 512] = jnp.dot(
                mixed[...],
                W[d % 2, d // 2, :, :, :, 0:512].reshape(1024, 512),
                preferred_element_type=F32,
            ).astype(BF16)
    with jax.named_scope("finish"):
        all_tiles(UT, us.at[0], ur.at[0]).wait_send()
        all_tiles(ASend, vs.at[0], vr.at[0]).wait_send()
        for ref, kind in (
            (W.at[0, pl.ds(0, 3), pl.ds(0, 5), 0], RING),
            (W.at[0, 0, pl.ds(0, 12)], NEAR),
            (W.at[0, pl.ds(0, 3)], BULK),
            (W.at[0], CORE),
        ):
            rcopy(ref, sends.at[kind], core.at[0], dev(cc=other)).wait_send()


def per_device(
    signal, pace, log_step, a_real, a_imag, in_map, out_map, skip, init_state, w_glu, b_glu, g_mix, w_out
):
    dma = pltpu.SemaphoreType.DMA
    anywhere = pl.BlockSpec(memory_space=pltpu.HBM)
    small = (
        jnp.swapaxes(in_map, 2, 3), out_map, skip[None], pace,
        log_step[None], a_real, a_imag, init_state, b_glu[None], g_mix[None],
    )
    return pl.pallas_call(
        body,
        out_shape=jax.ShapeDtypeStruct((1, 128, 4096), BF16),
        in_specs=[anywhere] * 13,
        out_specs=pl.BlockSpec(memory_space=pltpu.VMEM),
        scratch_shapes=[pltpu.VMEM(v.shape, v.dtype) for v in (signal, *small)]
        + [
            pltpu.VMEM((NC, NX, NZ, NY, 16, 640), BF16),
            pltpu.VMEM((SPN, 16, 128), BF16),
            pltpu.VMEM((SPN, 16, 128), BF16),
            pltpu.VMEM((4096, 128), F32),
            pltpu.VMEM((4096, 128), F32),
            pltpu.VMEM((SPN, 16, 128), BF16),
            pltpu.VMEM((SPN, 16, 128), BF16),
            pltpu.VMEM((32, 128), F32),
            pltpu.VMEM((32, 128), F32),
            pltpu.VMEM((128, 1024), BF16),
            pltpu.VMEM((128, 1024), F32),
            pltpu.VMEM((32, 256), F32),
            pltpu.VMEM((32, 256), F32),
            pltpu.VMEM((8, 256, 256), BF16),
            pltpu.VMEM((8, 256, 256), BF16),
            pltpu.VMEM((8, 128), F32),
            dma((13,)),
            dma((4,)),
            dma((9,)), dma((9,)),
            dma((8, 2)), dma((8, 2)), dma((8, 2)), dma((8, 2)),
            dma((1,)),
            dma((1,)), dma((1,)), dma((1,)), dma((1,)),
        ],
        compiler_params=pltpu.CompilerParams(
            collective_id=0, has_side_effects=True, vmem_limit_bytes=60 * 1024 * 1024
        ),
    )(signal, w_glu, w_out, *small)


def solution(mesh):
    split = Mesh(mesh.devices.reshape(NZ, NY, NX, NC), ("z", "y", "x", "c"))
    placed = (
        P(DP, SP, None),
        P(DP, None),
        P(SP),
        P(SP, None),
        P(SP, None),
        P(SP, None, None, None),
        P(SP, None, None, None),
        P(SP),
        P(DP, None, SP, None),
        P(SP, DP),
        P(),
        P(),
        P(SP, DP),
    )
    return jax.shard_map(
        per_device, mesh=split, in_specs=placed, out_specs=P(DP, SP, None), check_vma=False
    )
```
